32 devices in a mesh: ep: 8 (over z, x), tp: 4 (over y, core).
Axes of the slice: x: 2, y: 2, z: 4, core: 2. Of those that a mesh axis runs over, the one named last changes fastest.
Arguments:
- mixer_rows: bfloat16 [2048, 4096], P('ep'), may hold values from -8 to 8, as said below
- mixer_gain: float32 [4096], replicated, may hold values from 0.1 to 1.9
- gate_proj: bfloat16 [4096, 4096], P(None, 'tp'), may hold values from -0.09375 to 0.09375
- input_proj: bfloat16 [4096, 4096], P(None, 'tp'), may hold values from -0.09375 to 0.09375
- conv_taps: float32 [4, 4096], P(None, 'tp'), may hold values from -2 to 2
- input_gates: bfloat16 [16, 256, 256], P('tp'), may hold values from -0.375 to 0.375
- decay_gates: bfloat16 [16, 256, 256], P('tp'), may hold values from -0.375 to 0.375
- decay_offset: float32 [4096], P('tp'), may hold values from 4.8 to 13, as said below
- out_proj: bfloat16 [4096, 4096], P('tp'), may hold values from -0.09375 to 0.09375
- mixer_scale: float32 [4096], replicated, may hold values from 0.1 to 1.9
- expert_rows: bfloat16 [2048, 4096], P('ep'), may hold values from -6 to 6
- expert_gain: float32 [4096], replicated, may hold values from 0.1 to 1.9
- route_ids: int32 [2048, 2], P('ep'), may hold values from 0 to 7, all different within a row; in each aligned block of 256 rows (0 to 255, 256 to 511, ...) at most 96 rows name the same one
- route_weights: float32 [2048, 2], P('ep'), may hold values from 0.5 to 2
- expert_gate: bfloat16 [8, 4096, 1024], P('ep', None, 'tp'), may hold values from -0.09375 to 0.09375
- expert_up: bfloat16 [8, 4096, 1024], P('ep', None, 'tp'), may hold values from -0.09375 to 0.09375
- expert_down: bfloat16 [8, 1024, 4096], P('ep', 'tp'), may hold values from -0.1875 to 0.1875
- shared_gate: bfloat16 [4096, 1024], P(None, 'tp'), may hold values from -0.09375 to 0.09375
- shared_up: bfloat16 [4096, 1024], P(None, 'tp'), may hold values from -0.09375 to 0.09375
- shared_down: bfloat16 [1024, 4096], P('tp'), may hold values from -0.1875 to 0.1875
- expert_scale: float32 [4096], replicated, may hold values from 0.1 to 1.9
Outputs:
- mixer_out: bfloat16 [2048, 4096], P(('ep', 'tp'))
- expert_out: bfloat16 [2048, 4096], P(('ep', 'tp'))
The draws below stay inside these ranges and needn't reach their ends.
Inputs may be any that keep to these rules, and one draw needn't show every extreme that they name: `mixer_rows`: order one, with a common direction whose weight drifts slowly along the sequence. `decay_offset`: the even channels forget within some 30 to 200 tokens; the odd channels keep 5 to 90 percent of their state over the whole sequence of 2048 tokens. `route_ids`: each row names 2 different experts; within the rows of one index of ep (aligned blocks of 256 rows) no expert is named by more than 96 rows, and in some blocks one is named by exactly 96.
All inputs are finite; a program needn't handle non-finite values.
Results may differ from the reference program's by a relative error of at most 0.0033.
The reference program's roundings to bfloat16 on the way count: a program that leaves them out, or rounds other values in their place, can miss the bound.
Values may be sent and summed in bfloat16 or wider, within the bound.
A program may use at most 192 MiB of HBM per device.

```python
import math
import jax
import jax.numpy as jnp
import numpy as np
from jax import lax

D = 4096
RNN_BLOCKS = 16
BLOCK_WIDTH = 256
CONV = 4
EXPERT_HIDDEN = 1024
SHARED_HIDDEN = 1024
TOP_K = 2
ROWS = 256
EXPERTS = 8
TOKENS = 2048
CAP = 96
N_EP = 8


def draw_mixer_rows(key, part):
    noise_key, direction_key, phase_key = jax.random.split(key, 3)
    noise_part = jax.random.normal(noise_key, (TOKENS, D), jnp.float32)
    direction = jax.random.normal(direction_key, (D,), jnp.float32)
    phase_shift = jax.random.uniform(phase_key, (), jnp.float32, 0.0, 2.0 * math.pi)
    positions = jnp.arange(TOKENS, dtype=jnp.float32) / TOKENS
    drift_level = 2.0 * jnp.sin(3.0 * math.pi * positions + phase_shift)
    values = noise_part + drift_level[:, None] * direction[None, :]
    return jnp.clip(values, -8.0, 8.0).astype(jnp.bfloat16)


def draw_decay_offset(key, part):
    fast_key, slow_key = jax.random.split(key)
    fast_part = jax.random.uniform(fast_key, (D,), jnp.float32, 4.8, 6.7)
    slow_part = math.log(TOKENS) + jax.random.uniform(slow_key, (D,), jnp.float32, 0.3, 3.6)
    parity = jnp.arange(D) % 2
    return jnp.where(parity == 0, fast_part, slow_part).astype(jnp.float32)


def levels(key, dims, pieces, least, high):
    gain = 1.0
    for axis_at, shards_of in pieces:
        heights = jax.random.uniform(jax.random.fold_in(jax.random.fold_in(key, 6), axis_at), (shards_of,), jnp.float32, least / len(pieces), high / len(pieces))
        gain = gain * jnp.repeat(jnp.exp(heights), dims[axis_at] // shards_of).reshape((-1,) + (1,) * (len(dims) - 1 - axis_at))
    return gain


def routed_block(key, own, number, rows, amount, top, most, skew):
    order = jax.random.permutation(key, amount)
    crowded, common = portions_of(amount, rows * top, most, skew, True), portions_of(amount, rows * top, most, skew, False)
    places = jnp.arange(amount)

    def named(lengths, offset_by):
        used = int((lengths > 0).sum())
        fixed = max(1, used // 4)
        shifted = fixed + (places - fixed + offset_by * (used - fixed)) % max(1, amount - fixed)
        return jnp.zeros((amount,), jnp.int32).at[order[jnp.where(places < fixed, places, shifted)]].set(jnp.asarray(lengths, jnp.int32))

    lengths = jnp.where(number % 4 == 0, named(crowded, number // 4), named(common, number - number // 4 - 1))
    mixed = jax.random.permutation(jax.random.fold_in(own, 3), amount)
    donor, sink = mixed[0:amount // 2 * 2:2], mixed[1:amount // 2 * 2:2]
    room = jnp.minimum(lengths[donor] - 1, most - lengths[sink]) // 2
    room = jnp.where((donor == order[0]) | (sink == order[0]) | (lengths[sink] == 0), 0, jnp.maximum(room, 0))
    shifted = jax.random.randint(jax.random.fold_in(own, 4), (amount // 2,), 0, 1 << 20) % (room + 1)
    lengths = lengths.at[donor].add(-shifted).at[sink].add(shifted)
    members = jnp.searchsorted(jnp.cumsum(lengths), jnp.arange(rows * top), side="right").astype(jnp.int32)
    listing = members.reshape(top, rows).T
    listing = listing[jax.random.permutation(jax.random.fold_in(own, 1), rows)]
    offset_by = jax.random.randint(jax.random.fold_in(own, 2), (rows, 1), 0, top)
    return jnp.take_along_axis(listing, (jnp.arange(top)[None, :] + offset_by) % top, axis=1)


def portions_of(amount, total, bound, slope, full):
    portions = [(1 << 20) // math.isqrt(standing ** slope) + 1 for standing in range(1, amount + 1)]
    largest = bound if full else min(bound, max(-(-total // amount), total * portions[0] // sum(portions)))
    least = 1 if total - largest >= amount - 1 else 0
    counts, spare = [largest] + [least] * (amount - 1), total - largest - least * (amount - 1)
    while spare > 0:
        free = [i for i in range(1, amount) if counts[i] < largest] or [i for i in range(1, amount) if counts[i] < bound]
        whole, budget = sum([portions[i] for i in free]), spare
        for i in free:
            more = min(bound - counts[i], max(1, budget * portions[i] // whole), spare)
            counts[i] = counts[i] + more
            spare = spare - more
    return np.array(counts)


def centred(stream_key, shape, deviation, reach, cuts=(), kind=jnp.bfloat16):
    array = jax.random.normal(stream_key, shape, jnp.float32) * deviation
    if len(cuts) > 0:
        array = levels(stream_key, shape, cuts, -0.22, 0.18) * array
    return jnp.clip(array, min=-reach, max=reach).astype(kind)


def setup_inputs(seed: int = 0) -> dict:
    keys = jax.random.split(jax.random.key(seed), 22)
    mixer_rows = draw_mixer_rows(jax.random.fold_in(keys[21], 71), 0)
    mixer_gain = jnp.clip(1.0 + 0.18 * jax.random.normal(keys[1], (D,), jnp.float32), 0.1, 1.9)
    gate_proj = centred(keys[2], (D, D), D ** -0.5, 0.09375, ((1, 4),))
    input_proj = centred(keys[3], (D, D), D ** -0.5, 0.09375, ((1, 4),))
    conv_taps = centred(keys[4], (CONV, D), 0.5, 2.0, ((1, 4),), jnp.float32)
    input_gates = centred(keys[5], (RNN_BLOCKS, BLOCK_WIDTH, BLOCK_WIDTH), BLOCK_WIDTH ** -0.5, 0.375, ((0, 4),))
    decay_gates = centred(keys[6], (RNN_BLOCKS, BLOCK_WIDTH, BLOCK_WIDTH), BLOCK_WIDTH ** -0.5, 0.375, ((0, 4),))
    decay_offset = draw_decay_offset(jax.random.fold_in(keys[21], 71), 0)
    out_proj = centred(keys[8], (D, D), D ** -0.5, 0.09375, ((0, 4),))
    mixer_scale = jnp.clip(1.0 + 0.18 * jax.random.normal(keys[9], (D,), jnp.float32), 0.1, 1.9)
    expert_rows = centred(keys[10], (TOKENS, D), 1.0, 6.0, ((0, 8),))
    expert_gain = jnp.clip(1.0 + 0.18 * jax.random.normal(keys[11], (D,), jnp.float32), 0.1, 1.9)
    route_ids_keys = jax.random.split(jax.random.fold_in(keys[12], 1), TOKENS // ROWS)
    route_ids_turns = jax.random.permutation(jax.random.fold_in(keys[12], 3), TOKENS // ROWS)
    route_ids = jax.vmap(lambda own, number: routed_block(jax.random.fold_in(keys[12], 2), own, number, ROWS, EXPERTS, TOP_K, CAP, 1))(route_ids_keys, route_ids_turns).reshape((TOKENS, TOP_K))
    route_weights = jnp.clip(0.5 + 1.5 * jax.random.uniform(keys[13], (TOKENS, TOP_K), jnp.float32) ** levels(keys[13], (TOKENS, TOP_K), ((0, 8),), -0.2, 0.2), 0.5, 2.0)
    expert_gate = centred(keys[14], (EXPERTS, D, EXPERT_HIDDEN), D ** -0.5, 0.09375, ((0, 8), (2, 4)))
    expert_up = centred(keys[15], (EXPERTS, D, EXPERT_HIDDEN), D ** -0.5, 0.09375, ((0, 8), (2, 4)))
    expert_down = centred(keys[16], (EXPERTS, EXPERT_HIDDEN, D), EXPERT_HIDDEN ** -0.5, 0.1875, ((0, 8), (1, 4)))
    shared_gate = centred(keys[17], (D, SHARED_HIDDEN), D ** -0.5, 0.09375, ((1, 4),))
    shared_up = centred(keys[18], (D, SHARED_HIDDEN), D ** -0.5, 0.09375, ((1, 4),))
    shared_down = centred(keys[19], (SHARED_HIDDEN, D), SHARED_HIDDEN ** -0.5, 0.1875, ((0, 4),))
    expert_scale = jnp.clip(1.0 + 0.18 * jax.random.normal(keys[20], (D,), jnp.float32), 0.1, 1.9)
    return dict(mixer_rows=mixer_rows, mixer_gain=mixer_gain, gate_proj=gate_proj, input_proj=input_proj, conv_taps=conv_taps, input_gates=input_gates, decay_gates=decay_gates, decay_offset=decay_offset, out_proj=out_proj, mixer_scale=mixer_scale, expert_rows=expert_rows, expert_gain=expert_gain, route_ids=route_ids, route_weights=route_weights, expert_gate=expert_gate, expert_up=expert_up, expert_down=expert_down, shared_gate=shared_gate, shared_up=shared_up, shared_down=shared_down, expert_scale=expert_scale)


eps = 1e-06
lru_power = 8.0

def rms_scale(values, scale):
    floats = values.astype(jnp.float32)
    return floats * lax.rsqrt(lax.optimization_barrier(jnp.mean(floats * floats, axis=-1, keepdims=True)) + eps) * scale

def linear_pair(earlier, later):
    return (earlier[0] * later[0], later[0] * earlier[1] + later[1])

def slot_table(route_ids, expert_count, capacity):
    id_list = route_ids.reshape(-1).astype(jnp.int32)
    indicator = (id_list[:, None] == jnp.arange(expert_count, dtype=jnp.int32)[None, :]).astype(jnp.int32)
    earlier_count = (jnp.cumsum(indicator, axis=0).astype(jnp.int32) - indicator).astype(jnp.int32)
    position = lax.optimization_barrier(jnp.sum(earlier_count * indicator, axis=1)).astype(jnp.int32)
    slot_ids = (id_list * capacity + position).astype(jnp.int32)
    matched = (slot_ids[None, :] == jnp.arange(expert_count * capacity, dtype=jnp.int32)[:, None]).astype(jnp.int32)
    source = lax.optimization_barrier(jnp.sum(matched * jnp.arange(id_list.shape[0], dtype=jnp.int32)[None, :], axis=1)).astype(jnp.int32)
    filled = lax.optimization_barrier(jnp.sum(matched, axis=1)) > 0
    return (slot_ids, source, filled)

def mixer_half(mixer_rows, mixer_gain, gate_proj, input_proj, conv_taps, input_gates, decay_gates, decay_offset, out_proj, mixer_scale):
    row_count = mixer_rows.shape[0]
    normed = rms_scale(mixer_rows, mixer_gain).astype(jnp.bfloat16)
    gate_branch = jax.nn.gelu(jnp.dot(normed, gate_proj, preferred_element_type=jnp.float32))
    branch = jnp.dot(normed, input_proj, preferred_element_type=jnp.float32).astype(jnp.bfloat16)
    tap_count = conv_taps.shape[0]
    padded = jnp.concatenate([jnp.zeros((tap_count - 1, branch.shape[1]), branch.dtype), branch], axis=0)
    conv_sum = conv_taps[0] * padded[0:row_count].astype(jnp.float32)
    for tap_index in range(1, tap_count):
        conv_sum = conv_sum + conv_taps[tap_index] * padded[tap_index:tap_index + row_count].astype(jnp.float32)
    conv_out = conv_sum.astype(jnp.bfloat16)
    block_rows = conv_out.astype(jnp.float32).reshape(row_count, input_gates.shape[0], input_gates.shape[1])
    input_gate = jax.nn.sigmoid(jnp.einsum('rbi,bij->rbj', block_rows, input_gates.astype(jnp.float32))).reshape(row_count, -1)
    decay_gate = jax.nn.sigmoid(jnp.einsum('rbi,bij->rbj', block_rows, decay_gates.astype(jnp.float32))).reshape(row_count, -1)
    log_decay = -lru_power * decay_gate * jax.nn.softplus(-decay_offset)
    positions = jnp.arange(row_count, dtype=jnp.int32)
    input_scale = jnp.where((positions == 0)[:, None], 1.0, jnp.sqrt(-jnp.expm1(2.0 * log_decay)))
    drive_term = input_scale * input_gate * conv_out.astype(jnp.float32)
    decay_product, states = lax.associative_scan(linear_pair, (jnp.exp(log_decay), drive_term), axis=0)
    gated_rows = (gate_branch * states).astype(jnp.bfloat16)
    mixer_sum = jnp.dot(gated_rows, out_proj, preferred_element_type=jnp.float32)
    return rms_scale(mixer_sum, mixer_scale).astype(jnp.bfloat16)

def expert_half(expert_rows, expert_gain, route_ids, route_weights, expert_gate, expert_up, expert_down, shared_gate, shared_up, shared_down, expert_scale):
    expert_normed = rms_scale(expert_rows, expert_gain).astype(jnp.bfloat16)
    expert_count = expert_gate.shape[0]
    top_count = route_ids.shape[1]
    row_width = expert_rows.shape[1]
    gate_whole = expert_gate.astype(jnp.float32)
    up_whole = expert_up.astype(jnp.float32)
    down_whole = expert_down.astype(jnp.float32)

    def one_block(inputs):
        block_rows, block_ids, block_weights = inputs
        slot_ids, source, filled = slot_table(block_ids, expert_count, CAP)
        outgoing = jnp.where(filled[:, None], block_rows[source // top_count], jnp.zeros((), block_rows.dtype))
        outgoing = outgoing.reshape(expert_count, CAP, row_width).astype(jnp.float32)
        gate_part = jnp.einsum('ecd,edf->ecf', outgoing, gate_whole)
        up_part = jnp.einsum('ecd,edf->ecf', outgoing, up_whole)
        copy_hidden = (jax.nn.silu(gate_part) * up_part).astype(jnp.bfloat16)
        results = jnp.einsum('ecf,efd->ecd', copy_hidden.astype(jnp.float32), down_whole)
        picked = results.reshape(expert_count * CAP, row_width)[slot_ids] * block_weights.reshape(-1, 1)
        return lax.optimization_barrier(jnp.sum(picked.reshape(ROWS, top_count, row_width), axis=1))
    routed = lax.map(one_block, (expert_normed.reshape(N_EP, ROWS, row_width), route_ids.reshape(N_EP, ROWS, top_count), route_weights.reshape(N_EP, ROWS, top_count)))
    routed = routed.reshape(expert_rows.shape[0], row_width)
    shared_hidden = (jax.nn.silu(jnp.dot(expert_normed, shared_gate, preferred_element_type=jnp.float32)) * jnp.dot(expert_normed, shared_up, preferred_element_type=jnp.float32)).astype(jnp.bfloat16)
    expert_sum = routed + jnp.dot(shared_hidden, shared_down, preferred_element_type=jnp.float32)
    return rms_scale(expert_sum, expert_scale).astype(jnp.bfloat16)

def reference(mixer_rows, mixer_gain, gate_proj, input_proj, conv_taps, input_gates, decay_gates, decay_offset, out_proj, mixer_scale, expert_rows, expert_gain, route_ids, route_weights, expert_gate, expert_up, expert_down, shared_gate, shared_up, shared_down, expert_scale):
    mixer_out = mixer_half(mixer_rows, mixer_gain, gate_proj, input_proj, conv_taps, input_gates, decay_gates, decay_offset, out_proj, mixer_scale)
    expert_out = expert_half(expert_rows, expert_gain, route_ids, route_weights, expert_gate, expert_up, expert_down, shared_gate, shared_up, shared_down, expert_scale)
    return (mixer_out, expert_out)
```

```python
import functools

import jax
import jax.numpy as jnp
from jax import lax
from jax.experimental import pallas as pl
from jax.experimental.pallas import tpu as pltpu
from jax.sharding import PartitionSpec as P

eps = 1e-06
lru_power = 8.0
halo_rows = 16
MESH = pl.DeviceIdType.MESH
f32 = jnp.float32
bf16 = jnp.bfloat16


def rms_scale(values, scale):
    floats = values.astype(f32)
    return floats * lax.rsqrt(jnp.mean(floats * floats, axis=-1, keepdims=True) + eps) * scale


def remote(src, dst, send_sem, recv_sem, ep_at, tp_at):
    return pltpu.make_async_remote_copy(
        src_ref=src,
        dst_ref=dst,
        send_sem=send_sem,
        recv_sem=recv_sem,
        device_id=(ep_at, tp_at),
        device_id_type=MESH,
    )


def greet(peers):
    barrier = pltpu.get_barrier_semaphore()
    for ep_at, tp_at in peers:
        pl.semaphore_signal(barrier, inc=1, device_id=(ep_at, tp_at), device_id_type=MESH)
    pl.semaphore_wait(barrier, len(peers))


def expm1_neg(y):
    series = y * (1 + y / 2 * (1 + y / 3 * (1 + y / 4 * (1 + y / 5 * (1 + y / 6 * (1 + y / 7))))))
    return jnp.where(y > -0.35, series, jnp.exp(y) - 1.0)


def mixer_kernel(
    ep, branch_ref, gate_ref, taps_ref, ig_ref, dg_ref, soft_ref, out_ref,
    ext, halo, a_buf, b_buf, ends, got, halo_send, halo_recv, end_send, end_recv,
):
    me, t = lax.axis_index("ep"), lax.axis_index("tp")
    rows, width = branch_ref.shape
    blocks, bw = ig_ref.shape[0], ig_ref.shape[1]
    greet([(lax.rem(me + i, ep), t) for i in range(1, ep)])
    nxt = remote(
        branch_ref.at[pl.ds(rows - halo_rows, halo_rows)], halo,
        halo_send, halo_recv, lax.rem(me + 1, ep), t,
    )
    nxt.start()
    ext[pl.ds(halo_rows, rows), :] = branch_ref[...].astype(f32)
    nxt.wait()
    ext[pl.ds(0, halo_rows), :] = jnp.where(me == 0, 0.0, halo[...].astype(f32))
    taps = taps_ref.shape[0]
    base = halo_rows - (taps - 1)
    first = (lax.broadcasted_iota(jnp.int32, (rows, bw), 0) == 0) & (me == 0)
    for b in range(blocks):
        cols = pl.ds(b * bw, bw)
        acc = taps_ref[0:1, cols] * ext[pl.ds(base, rows), cols]
        for k in range(1, taps):
            acc = acc + taps_ref[k : k + 1, cols] * ext[pl.ds(base + k, rows), cols]
        conv = acc.astype(bf16)
        ig = jax.nn.sigmoid(jnp.dot(conv, ig_ref[b], preferred_element_type=f32))
        dg = jax.nn.sigmoid(jnp.dot(conv, dg_ref[b], preferred_element_type=f32))
        ld = -lru_power * dg * soft_ref[0:1, cols]
        scale = jnp.where(first, 1.0, jnp.sqrt(-expm1_neg(2.0 * ld)))
        a_buf[:, cols] = jnp.exp(ld)
        b_buf[:, cols] = scale * ig * conv.astype(f32)

    row = lax.broadcasted_iota(jnp.int32, (8, width), 0)

    def block(r, carry):
        pc, sc = carry
        at = pl.ds(pl.multiple_of(r * 8, 8), 8)
        a, b = a_buf[at, :], b_buf[at, :]
        for sh in (1, 2, 4):
            keep = row >= sh
            b = jnp.where(keep, b + a * pltpu.roll(b, sh, 0), b)
            a = jnp.where(keep, a * pltpu.roll(a, sh, 0), a)
        b = b + a * sc
        a = a * pc
        a_buf[at, :] = a
        b_buf[at, :] = b
        return a[7:8, :], b[7:8, :]

    pl_last, s_last = lax.fori_loop(
        0, rows // 8, block, (jnp.ones((1, width), f32), jnp.zeros((1, width), f32))
    )
    ends[...] = jnp.where(row == 0, pl_last, s_last)
    copies = [
        remote(ends, got.at[i], end_send.at[i], end_recv.at[i], lax.rem(me + i, ep), t)
        for i in range(1, ep)
    ]
    for c in copies:
        c.start()
    for c in copies:
        c.wait()
    carry = jnp.zeros((1, width), f32)
    for i in range(ep - 1, 0, -1):
        carry = jnp.where(me >= i, got[i, 0:1, :] * carry + got[i, 1:2, :], carry)

    def finish(r, _):
        at = pl.ds(pl.multiple_of(r * 16, 16), 16)
        out_ref[at, :] = (gate_ref[at, :] * (b_buf[at, :] + a_buf[at, :] * carry)).astype(bf16)
        return 0

    lax.fori_loop(0, rows // 16, finish, 0)


def moe_kernel(
    ep, tp, outq, eg_hbm, eu_hbm, ed, back,
    recv, eg, eu, wd, hid, ret, load_sem,
    z_s, z_r, y_s, y_r, c_s, c_r, hy_s, hy_r, hc_s, hc_r, w_s, w_r, b_s, b_r,
):
    me, t = lax.axis_index("ep"), lax.axis_index("tp")
    ys = tp // 2
    y, c = t // 2, lax.rem(t, 2)
    mate = y * 2 + 1 - c
    dq = outq.shape[2]

    def up(k):
        return lax.rem(y + k, ys) * 2 + c

    def down_of(k, core):
        return lax.rem(y + ys - k, ys) * 2 + core

    greet(
        [(lax.rem(me + i, ep), t) for i in range(1, ep)]
        + [(me, lax.rem(t + i, tp)) for i in range(1, tp)]
    )

    def z_copy(i):
        return remote(
            outq.at[i], recv.at[t, i], z_s.at[i], z_r.at[i], lax.rem(me + i, ep), t
        )

    def y_copy(k, i):
        return remote(recv.at[t, i], recv.at[t, i], y_s.at[k, i], y_r.at[k, i], me, up(k))

    def c_copy(k, i):
        q = down_of(k, c)
        return remote(recv.at[q, i], recv.at[q, i], c_s.at[k, i], c_r.at[k, i], me, mate)

    def hy_copy(k, i):
        return remote(hid.at[t, i], hid.at[t, i], hy_s.at[k, i], hy_r.at[k, i], me, up(k))

    def hc_copy(k, i):
        q = down_of(k, c)
        return remote(hid.at[q, i], hid.at[q, i], hc_s.at[k, i], hc_r.at[k, i], me, mate)

    def w_copy(i):
        q = lax.rem(t + i, tp)
        return remote(
            ed.at[:, pl.ds(pl.multiple_of(q * dq, dq), dq)], wd.at[t],
            w_s.at[i], w_r.at[i], me, q,
        )

    def b_copy(i):
        return remote(
            ret.at[i], back.at[i], b_s.at[i], b_r.at[i], lax.rem(me + ep - i, ep), t
        )

    for i in range(1, ep):
        z_copy(i).start()
    loads = [
        pltpu.make_async_copy(outq.at[0], recv.at[t, 0], load_sem.at[0]),
        pltpu.make_async_copy(eg_hbm, eg, load_sem.at[1]),
        pltpu.make_async_copy(eu_hbm, eu, load_sem.at[2]),
        pltpu.make_async_copy(
            ed.at[:, pl.ds(pl.multiple_of(t * dq, dq), dq)], wd.at[t], load_sem.at[3]
        ),
    ]
    for load in loads:
        load.start()
    for load in loads:
        load.wait()

    def step(n, _):
        @pl.when(n < ep)
        def _():
            i = n

            @pl.when(i > 0)
            def _():
                z_copy(i).wait_recv()

            for k in range(1, ys):
                y_copy(k, i).start()
            c_copy(0, i).start()

        @pl.when(n == 1)
        def _():
            for i in range(1, tp):
                w_copy(i).start()

        @pl.when((n >= 1) & (n < ep + 1))
        def _():
            i = n - 1
            for k in range(1, ys):
                y_copy(k, i).wait_recv()
                c_copy(k, i).start()

        @pl.when((n >= 2) & (n < ep + 2))
        def _():
            i = n - 2
            for k in range(ys):
                c_copy(k, i).wait_recv()
            gate = up_sum = None
            for q in range(tp):
                x = recv[q, i]
                span = pl.ds(q * dq, dq)
                g = jnp.dot(x, eg[span, :], preferred_element_type=f32)
                u = jnp.dot(x, eu[span, :], preferred_element_type=f32)
                gate = g if gate is None else gate + g
                up_sum = u if up_sum is None else up_sum + u
            hid[t, i] = (jax.nn.silu(gate) * up_sum).astype(bf16)
            for k in range(1, ys):
                hy_copy(k, i).start()
            hc_copy(0, i).start()

        @pl.when((n >= 3) & (n < ep + 3))
        def _():
            i = n - 3
            for k in range(1, ys):
                hy_copy(k, i).wait_recv()
                hc_copy(k, i).start()

        @pl.when(n == 4)
        def _():
            for i in range(1, tp):
                w_copy(i).wait()

        @pl.when(n >= 4)
        def _():
            i = n - 4
            for k in range(ys):
                hc_copy(k, i).wait_recv()
            total = jnp.dot(hid[0, i], wd[0], preferred_element_type=f32)
            for q in range(1, tp):
                total = total + jnp.dot(hid[q, i], wd[q], preferred_element_type=f32)

            @pl.when(i == 0)
            def _():
                back[0] = total.astype(bf16)

            @pl.when(i > 0)
            def _():
                ret[i] = total.astype(bf16)
                b_copy(i).start()

        return 0

    lax.fori_loop(0, ep + 4, step, 0)

    def settle(i, _):
        for k in range(1, ys):
            y_copy(k, i).wait_send()
            hy_copy(k, i).wait_send()
        for k in range(ys):
            c_copy(k, i).wait_send()
            hc_copy(k, i).wait_send()

        @pl.when(i > 0)
        def _():
            z_copy(i).wait_send()
            b_copy(i).wait()

        return 0

    lax.fori_loop(0, ep, settle, 0)


def final_kernel(
    tp, m_ref, e_ref, ms_ref, es_ref, mo_ref, eo_ref,
    m_half, e_half, m_out, m_in, e_in, md_s, md_r, ed_s, ed_r, my_s, my_r, ey_s, ey_r,
):
    me, t = lax.axis_index("ep"), lax.axis_index("tp")
    ys = tp // 2
    y, c = t // 2, lax.rem(t, 2)
    mate = y * 2 + 1 - c

    def at_y(k):
        return lax.rem(y + k, ys)

    greet([(me, mate)] + [(me, at_y(k) * 2 + c) for k in range(1, ys)])
    order = list(range(1, ys)) + [0]

    def pair(ref, half, s, r, k):
        q = at_y(k) * 2 + 1 - c
        return remote(ref.at[q], half.at[k], s.at[k], r.at[k], me, mate)

    for k in order:
        pair(m_ref, m_half, md_s, md_r, k).start()
    for k in order:
        pair(e_ref, e_half, ed_s, ed_r, k).start()

    def my_copy(k):
        return remote(m_out.at[k], m_in.at[k], my_s.at[k], my_r.at[k], me, at_y(k) * 2 + c)

    def ey_copy(k):
        return remote(e_half.at[k], e_in.at[k], ey_s.at[k], ey_r.at[k], me, at_y(k) * 2 + c)

    for k in range(1, ys):
        pair(m_ref, m_half, md_s, md_r, k).wait_recv()
        m_out[k] = (m_half[k] + m_ref[at_y(k) * 2 + c]).astype(bf16)
        my_copy(k).start()
    for k in range(1, ys):
        pair(e_ref, e_half, ed_s, ed_r, k).wait_recv()
        e_half[k] = e_half[k] + e_ref[at_y(k) * 2 + c]
        ey_copy(k).start()
    pair(m_ref, m_half, md_s, md_r, 0).wait_recv()
    total = m_half[0] + m_ref[t]
    for k in range(1, ys):
        my_copy(k).wait_recv()
        total = total + m_in[k].astype(f32)
    mo_ref[...] = rms_scale(total, ms_ref[...]).astype(bf16)
    pair(e_ref, e_half, ed_s, ed_r, 0).wait_recv()
    total = e_half[0] + e_ref[t]
    for k in range(1, ys):
        ey_copy(k).wait_recv()
        total = total + e_in[k]
    eo_ref[...] = rms_scale(total, es_ref[...]).astype(bf16)
    for k in range(ys):
        pair(m_ref, m_half, md_s, md_r, k).wait_send()
        pair(e_ref, e_half, ed_s, ed_r, k).wait_send()
    for k in range(1, ys):
        my_copy(k).wait_send()
        ey_copy(k).wait_send()


def vmem(n):
    return [pl.BlockSpec(memory_space=pltpu.VMEM)] * n


def dma(*shape):
    return pltpu.SemaphoreType.DMA(shape)


def params(number):
    return pltpu.CompilerParams(
        collective_id=number, has_side_effects=True, vmem_limit_bytes=60 * 1024 * 1024
    )


def recurrence(ep, branch, gate_branch, conv_taps, input_gates, decay_gates, soft):
    rows, width = branch.shape
    return pl.pallas_call(
        functools.partial(mixer_kernel, ep),
        out_shape=jax.ShapeDtypeStruct((rows, width), bf16),
        in_specs=vmem(6),
        out_specs=vmem(1)[0],
        scratch_shapes=[
            pltpu.VMEM((halo_rows + rows, width), f32),
            pltpu.VMEM((halo_rows, width), bf16),
            pltpu.VMEM((rows, width), f32),
            pltpu.VMEM((rows, width), f32),
            pltpu.VMEM((8, width), f32),
            pltpu.VMEM((ep, 8, width), f32),
            pltpu.SemaphoreType.DMA,
            pltpu.SemaphoreType.DMA,
            dma(ep),
            dma(ep),
        ],
        compiler_params=params(0),
        name="recurrence",
    )(branch, gate_branch, conv_taps, input_gates, decay_gates, soft)


def experts(ep, tp, outq, expert_gate, expert_up, expert_down):
    _, cap, dq = outq.shape
    depth, hf = expert_gate.shape
    ys = tp // 2
    return pl.pallas_call(
        functools.partial(moe_kernel, ep, tp),
        out_shape=jax.ShapeDtypeStruct((ep, cap, dq), bf16),
        in_specs=vmem(1) + [pl.BlockSpec(memory_space=pl.ANY)] * 3,
        out_specs=vmem(1)[0],
        scratch_shapes=[
            pltpu.VMEM((tp, ep, cap, dq), bf16),
            pltpu.VMEM((depth, hf), bf16),
            pltpu.VMEM((depth, hf), bf16),
            pltpu.VMEM((tp, hf, dq), bf16),
            pltpu.VMEM((tp, ep, cap, hf), bf16),
            pltpu.VMEM((ep, cap, dq), bf16),
            dma(4),
            dma(ep), dma(ep),
            dma(ys, ep), dma(ys, ep),
            dma(ys, ep), dma(ys, ep),
            dma(ys, ep), dma(ys, ep),
            dma(ys, ep), dma(ys, ep),
            dma(tp), dma(tp),
            dma(ep), dma(ep),
        ],
        compiler_params=params(1),
        name="experts",
    )(outq, expert_gate, expert_up, expert_down)


def final(tp, mixer_term, expert_term, mixer_scale, expert_scale):
    rows, width = mixer_term.shape
    each, ys = rows // tp, tp // 2
    return pl.pallas_call(
        functools.partial(final_kernel, tp),
        out_shape=[jax.ShapeDtypeStruct((each, width), bf16)] * 2,
        in_specs=vmem(4),
        out_specs=vmem(2),
        scratch_shapes=[
            pltpu.VMEM((ys, each, width), f32),
            pltpu.VMEM((ys, each, width), f32),
            pltpu.VMEM((ys, each, width), bf16),
            pltpu.VMEM((ys, each, width), bf16),
            pltpu.VMEM((ys, each, width), f32),
            dma(ys), dma(ys), dma(ys), dma(ys),
            dma(ys), dma(ys), dma(ys), dma(ys),
        ],
        compiler_params=params(2),
        name="final",
    )(
        mixer_term.reshape(tp, each, width),
        expert_term.reshape(tp, each, width),
        mixer_scale.reshape(1, -1),
        expert_scale.reshape(1, -1),
    )


def body(
    mixer_rows, mixer_gain, gate_proj, input_proj, conv_taps, input_gates, decay_gates,
    decay_offset, out_proj, mixer_scale, expert_rows, expert_gain, route_ids, route_weights,
    expert_gate, expert_up, expert_down, shared_gate, shared_up, shared_down, expert_scale,
):
    ep, tp = lax.axis_size("ep"), lax.axis_size("tp")
    me, t = lax.axis_index("ep"), lax.axis_index("tp")
    tokens, width = expert_rows.shape
    top = route_ids.shape[1]
    cap = tokens * top * 3 // (2 * ep)
    dq = width // tp

    expert_normed = rms_scale(expert_rows, expert_gain).astype(bf16)
    offset_ids = lax.rem(route_ids + (ep - me), ep)
    indicator = jnp.sum(
        (offset_ids[:, :, None] == jnp.arange(ep, dtype=jnp.int32)).astype(f32), axis=1
    )
    below = (
        jnp.arange(tokens)[:, None] > jnp.arange(tokens)[None, :]
    ).astype(bf16)
    earlier = jnp.dot(below, indicator.astype(bf16), preferred_element_type=f32)
    chosen = (offset_ids[:, :, None] == jnp.arange(ep, dtype=jnp.int32)).astype(f32)
    position = jnp.sum(chosen * earlier[:, None, :], axis=2).astype(jnp.int32)
    slot_ids = offset_ids * cap + position
    slots = jnp.arange(ep * cap, dtype=jnp.int32)
    picks = [(slot_ids[:, k][:, None] == slots[None, :]).astype(bf16) for k in range(top)]
    placed = sum(picks[1:], picks[0])
    quarter = lax.dynamic_slice_in_dim(expert_normed, t * dq, dq, axis=1)
    outq = lax.dot_general(
        placed, quarter, (((0,), (0,)), ((), ())), preferred_element_type=f32
    ).astype(bf16).reshape(ep, cap, dq)
    back = experts(ep, tp, outq, expert_gate[0], expert_up[0], expert_down[0])

    normed = rms_scale(mixer_rows, mixer_gain).astype(bf16)
    gate_branch = jax.nn.gelu(jnp.dot(normed, gate_proj, preferred_element_type=f32))
    branch = jnp.dot(normed, input_proj, preferred_element_type=f32).astype(bf16)
    soft = jax.nn.softplus(-decay_offset).reshape(1, -1)
    gated = recurrence(ep, branch, gate_branch, conv_taps, input_gates, decay_gates, soft)
    mixer_term = jnp.dot(gated, out_proj, preferred_element_type=f32)

    shared_hidden = (
        jax.nn.silu(jnp.dot(expert_normed, shared_gate, preferred_element_type=f32))
        * jnp.dot(expert_normed, shared_up, preferred_element_type=f32)
    ).astype(bf16)
    shared_term = jnp.dot(shared_hidden, shared_down, preferred_element_type=f32)
    flat = back.reshape(ep * cap, dq)
    routed = sum(
        route_weights[:, k : k + 1] * jnp.dot(picks[k], flat, preferred_element_type=f32)
        for k in range(top)
    )
    mine = lax.dynamic_slice_in_dim(shared_term, t * dq, dq, axis=1)
    expert_term = lax.dynamic_update_slice_in_dim(shared_term, mine + routed, t * dq, axis=1)
    return tuple(final(tp, mixer_term, expert_term, mixer_scale, expert_scale))


def solution(mesh):
    placed = (
        P("ep", None),
        P(),
        P(None, "tp"),
        P(None, "tp"),
        P(None, "tp"),
        P("tp", None, None),
        P("tp", None, None),
        P("tp"),
        P("tp", None),
        P(),
        P("ep", None),
        P(),
        P("ep", None),
        P("ep", None),
        P("ep", None, "tp"),
        P("ep", None, "tp"),
        P("ep", "tp", None),
        P(None, "tp"),
        P(None, "tp"),
        P("tp", None),
        P(),
    )
    return jax.shard_map(
        body,
        mesh=mesh,
        in_specs=placed,
        out_specs=(P(("ep", "tp"), None), P(("ep", "tp"), None)),
        check_vma=False,
    )
```

```python
import functools

import jax
import jax.numpy as jnp
from jax import lax
from jax.experimental import pallas as pl
from jax.experimental.pallas import tpu as pltpu
from jax.sharding import PartitionSpec as P

eps = 1e-06
lru_power = 8.0
halo_rows = 16
MESH = pl.DeviceIdType.MESH
f32 = jnp.float32
bf16 = jnp.bfloat16


def rms_scale(values, scale):
    floats = values.astype(f32)
    return floats * lax.rsqrt(jnp.mean(floats * floats, axis=-1, keepdims=True) + eps) * scale


def remote(src, dst, send_sem, recv_sem, ep_at, tp_at):
    return pltpu.make_async_remote_copy(
        src_ref=src,
        dst_ref=dst,
        send_sem=send_sem,
        recv_sem=recv_sem,
        device_id=(ep_at, tp_at),
        device_id_type=MESH,
    )


def greet(peers):
    barrier = pltpu.get_barrier_semaphore()
    for ep_at, tp_at in peers:
        pl.semaphore_signal(barrier, inc=1, device_id=(ep_at, tp_at), device_id_type=MESH)
    pl.semaphore_wait(barrier, len(peers))


def expm1_neg(y):
    series = y * (1 + y / 2 * (1 + y / 3 * (1 + y / 4 * (1 + y / 5 * (1 + y / 6 * (1 + y / 7))))))
    return jnp.where(y > -0.35, series, jnp.exp(y) - 1.0)


def layer_kernel(
    ep, tp, top,
    outq, normed, en, taps_ref, ig_ref, dg_ref, soft_ref, picks, weights, ms_ref, es_ref,
    ip_hbm, gp_hbm, op_hbm, eg_hbm, eu_hbm, ed, sg_hbm, su_hbm, sd_hbm,
    mo_ref, eo_ref,
    w1, eg, eu, wd, sd, recv, hid, ret, back, mt, st, m_half, e_half, m_out, m_in, e_in,
    r_buf, r_in, total, gate, a_buf, b_buf, ext, tail, halo, ends, got, gated,
    load_sem, halo_send, halo_recv, end_send, end_recv,
    z_s, z_r, y_s, y_r, c_s, c_r, hy_s, hy_r, hc_s, hc_r, w_s, w_r, b_s, b_r,
    md_s, md_r, ed_s, ed_r, my_s, my_r, ey_s, ey_r, r_s, r_r,
):
    me, t = lax.axis_index("ep"), lax.axis_index("tp")
    ys = tp // 2
    y, c = t // 2, lax.rem(t, 2)
    mate = y * 2 + 1 - c
    dq = outq.shape[2]
    rows, width = ext.shape[0] - halo_rows, ext.shape[1]
    each = rows // tp
    blocks, bw = ig_ref.shape[0], ig_ref.shape[1]
    sh_width = sd.shape[0]

    def at_y(k):
        return lax.rem(y + k, ys)

    def up(k):
        return at_y(k) * 2 + c

    def down_of(k, core):
        return lax.rem(y + ys - k, ys) * 2 + core

    greet(
        [(lax.rem(me + i, ep), t) for i in range(1, ep)]
        + [(me, lax.rem(t + i, tp)) for i in range(1, tp)]
    )

    def z_copy(i):
        return remote(
            outq.at[i], recv.at[t, i], z_s.at[i], z_r.at[i], lax.rem(me + i, ep), t
        )

    def y_copy(k, i):
        return remote(recv.at[t, i], recv.at[t, i], y_s.at[k, i], y_r.at[k, i], me, up(k))

    def c_copy(k, i):
        q = down_of(k, c)
        return remote(recv.at[q, i], recv.at[q, i], c_s.at[k, i], c_r.at[k, i], me, mate)

    def hy_copy(k, i):
        return remote(hid.at[t, i], hid.at[t, i], hy_s.at[k, i], hy_r.at[k, i], me, up(k))

    def hc_copy(k, i):
        q = down_of(k, c)
        return remote(hid.at[q, i], hid.at[q, i], hc_s.at[k, i], hc_r.at[k, i], me, mate)

    def w_copy(i):
        q = lax.rem(t + i, tp)
        return remote(
            ed.at[:, pl.ds(pl.multiple_of(q * dq, dq), dq)], wd.at[t],
            w_s.at[i], w_r.at[i], me, q,
        )

    def b_copy(i):
        return remote(
            ret.at[i], back.at[i], b_s.at[i], b_r.at[i], lax.rem(me + ep - i, ep), t
        )

    def halo_copy():
        return remote(tail, halo, halo_send, halo_recv, lax.rem(me + 1, ep), t)

    def end_copy(i):
        return remote(ends, got.at[i], end_send.at[i], end_recv.at[i], lax.rem(me + i, ep), t)

    def pair(ref, half, s, r, k):
        return remote(ref.at[at_y(k) * 2 + 1 - c], half.at[k], s.at[k], r.at[k], me, mate)

    def my_copy(k):
        return remote(m_out.at[k], m_in.at[k], my_s.at[k], my_r.at[k], me, up(k))

    def ey_copy(k):
        return remote(e_half.at[k], e_in.at[k], ey_s.at[k], ey_r.at[k], me, up(k))

    def r_copy(i):
        q = lax.rem(t + i, tp)
        return remote(r_buf.at[q], r_in.at[t], r_s.at[i], r_r.at[i], me, q)

    def load(src, dst, at):
        return pltpu.make_async_copy(src, dst, load_sem.at[at])

    for i in range(1, ep):
        z_copy(i).start()
    own_rows = load(outq.at[0], recv.at[t, 0], 0)
    own_rows.start()
    ip_load = load(ip_hbm, w1, 1)
    ip_load.start()
    eg_load, eu_load = load(eg_hbm, eg, 2), load(eu_hbm, eu, 3)
    eg_load.start()
    eu_load.start()
    wd_load = load(ed.at[:, pl.ds(pl.multiple_of(t * dq, dq), dq)], wd.at[t], 4)
    wd_load.start()
    sd_load = load(sd_hbm, sd, 5)
    sd_load.start()
    sg_load = load(sg_hbm, w1.at[:, pl.ds(0, sh_width)], 6)
    su_load = load(su_hbm, w1.at[:, pl.ds(sh_width, sh_width)], 7)
    gp_load = load(gp_hbm, w1, 8)
    op_loads = [
        load(op_hbm.at[:, pl.ds(q * dq, dq)], w1.at[pl.ds(q * width, width), :], 9 + q)
        for q in range(tp)
    ]
    own_rows.wait()

    def project():
        ip_load.wait()

        def columns(j, _):
            cols = pl.ds(pl.multiple_of(j * bw, bw), bw)
            piece = jnp.dot(normed[...], w1[:, cols], preferred_element_type=f32).astype(bf16)
            ext[pl.ds(halo_rows, rows), cols] = piece.astype(f32)
            tail[:, cols] = piece[rows - halo_rows :]
            return 0

        lax.fori_loop(0, width // bw, columns, 0)
        halo_copy().start()
        sg_load.start()
        su_load.start()

    def shared():
        sg_load.wait()
        su_load.wait()
        g = jnp.dot(en[...], w1[:, pl.ds(0, sh_width)], preferred_element_type=f32)
        u = jnp.dot(en[...], w1[:, pl.ds(sh_width, sh_width)], preferred_element_type=f32)
        hidden = (jax.nn.silu(g) * u).astype(bf16)
        gp_load.start()
        sd_load.wait()
        for q in range(tp):
            cols = pl.ds(q * dq, dq)
            piece = jnp.dot(hidden, sd[:, cols], preferred_element_type=f32)
            st[:, :, cols] = piece.reshape(tp, each, dq)

    def gate_step():
        gp_load.wait()

        def columns(j, _):
            cols = pl.ds(pl.multiple_of(j * bw, bw), bw)
            piece = jnp.dot(normed[...], w1[:, cols], preferred_element_type=f32)
            gate[:, cols] = jax.nn.gelu(piece)
            return 0

        lax.fori_loop(0, width // bw, columns, 0)
        for one in op_loads:
            one.start()

    def convolve():
        halo_copy().wait()
        ext[pl.ds(0, halo_rows), :] = jnp.where(me == 0, 0.0, halo[...].astype(f32))
        taps = taps_ref.shape[0]
        base = halo_rows - (taps - 1)
        first = (lax.broadcasted_iota(jnp.int32, (rows, bw), 0) == 0) & (me == 0)
        for b in range(blocks):
            cols = pl.ds(b * bw, bw)
            acc = taps_ref[0:1, cols] * ext[pl.ds(base, rows), cols]
            for k in range(1, taps):
                acc = acc + taps_ref[k : k + 1, cols] * ext[pl.ds(base + k, rows), cols]
            conv = acc.astype(bf16)
            ig = jax.nn.sigmoid(jnp.dot(conv, ig_ref[b], preferred_element_type=f32))
            dg = jax.nn.sigmoid(jnp.dot(conv, dg_ref[b], preferred_element_type=f32))
            ld = -lru_power * dg * soft_ref[0:1, cols]
            scale = jnp.where(first, 1.0, jnp.sqrt(-expm1_neg(2.0 * ld)))
            a_buf[:, cols] = jnp.exp(ld)
            b_buf[:, cols] = scale * ig * conv.astype(f32)

    def scan():
        row = lax.broadcasted_iota(jnp.int32, (8, width), 0)

        def block(r, carry):
            pc, sc = carry
            at = pl.ds(pl.multiple_of(r * 8, 8), 8)
            a, b = a_buf[at, :], b_buf[at, :]
            for sh in (1, 2, 4):
                keep = row >= sh
                b = jnp.where(keep, b + a * pltpu.roll(b, sh, 0), b)
                a = jnp.where(keep, a * pltpu.roll(a, sh, 0), a)
            b = b + a * sc
            a = a * pc
            a_buf[at, :] = a
            b_buf[at, :] = b
            return a[7:8, :], b[7:8, :]

        pl_last, s_last = lax.fori_loop(
            0, rows // 8, block, (jnp.ones((1, width), f32), jnp.zeros((1, width), f32))
        )
        ends[...] = jnp.where(row == 0, pl_last, s_last)
        for i in range(1, ep):
            end_copy(i).start()

    def carry_in():
        for i in range(1, ep):
            end_copy(i).wait()
        carry = jnp.zeros((1, width), f32)
        for i in range(ep - 1, 0, -1):
            carry = jnp.where(me >= i, got[i, 0:1, :] * carry + got[i, 1:2, :], carry)

        def finish(r, _):
            at = pl.ds(pl.multiple_of(r * 16, 16), 16)
            gated[at, :] = (gate[at, :] * (b_buf[at, :] + a_buf[at, :] * carry)).astype(bf16)
            return 0

        lax.fori_loop(0, rows // 16, finish, 0)

    def project_out():
        for one in op_loads:
            one.wait()
        for q in range(tp):
            piece = jnp.dot(
                gated[...], w1[pl.ds(q * width, width), :], preferred_element_type=f32
            )
            mt[:, :, pl.ds(q * dq, dq)] = piece.reshape(tp, each, dq)
        for k in range(ys):
            pair(mt, m_half, md_s, md_r, k).start()
        for k in range(ys):
            pair(st, e_half, ed_s, ed_r, k).start()

    def halves():
        for k in range(1, ys):
            pair(mt, m_half, md_s, md_r, k).wait_recv()
            m_out[k] = (m_half[k] + mt[up(k)]).astype(bf16)
            my_copy(k).start()
        for k in range(1, ys):
            pair(st, e_half, ed_s, ed_r, k).wait_recv()
            e_half[k] = e_half[k] + st[up(k)]
            ey_copy(k).start()

    work = {
        0: project, 1: shared, 2: gate_step, 3: convolve, 4: scan, 5: carry_in, 6: project_out,
        ep + 2: halves,
    }

    def step(n, _):
        @pl.when(n < ep)
        def _():
            i = n

            @pl.when(i > 0)
            def _():
                z_copy(i).wait_recv()

            for k in range(1, ys):
                y_copy(k, i).start()
            c_copy(0, i).start()

        @pl.when(n == 1)
        def _():
            for i in range(1, tp):
                w_copy(i).start()

        @pl.when((n >= 1) & (n < ep + 1))
        def _():
            i = n - 1
            for k in range(1, ys):
                y_copy(k, i).wait_recv()
                c_copy(k, i).start()

        @pl.when(n == 2)
        def _():
            eg_load.wait()
            eu_load.wait()

        @pl.when((n >= 2) & (n < ep + 2))
        def _():
            i = n - 2
            for k in range(ys):
                c_copy(k, i).wait_recv()
            gate_sum = up_sum = None
            for q in range(tp):
                x = recv[q, i]
                span = pl.ds(q * dq, dq)
                g = jnp.dot(x, eg[span, :], preferred_element_type=f32)
                u = jnp.dot(x, eu[span, :], preferred_element_type=f32)
                gate_sum = g if gate_sum is None else gate_sum + g
                up_sum = u if up_sum is None else up_sum + u
            hid[t, i] = (jax.nn.silu(gate_sum) * up_sum).astype(bf16)
            for k in range(1, ys):
                hy_copy(k, i).start()
            hc_copy(0, i).start()

        @pl.when((n >= 3) & (n < ep + 3))
        def _():
            i = n - 3
            for k in range(1, ys):
                hy_copy(k, i).wait_recv()
                hc_copy(k, i).start()

        @pl.when(n == 4)
        def _():
            wd_load.wait()
            for i in range(1, tp):
                w_copy(i).wait()

        @pl.when(n >= 4)
        def _():
            i = n - 4
            for k in range(ys):
                hc_copy(k, i).wait_recv()
            out = jnp.dot(hid[0, i], wd[0], preferred_element_type=f32)
            for q in range(1, tp):
                out = out + jnp.dot(hid[q, i], wd[q], preferred_element_type=f32)

            @pl.when(i == 0)
            def _():
                back[0] = out.astype(bf16)

            @pl.when(i > 0)
            def _():
                ret[i] = out.astype(bf16)
                b_copy(i).start()

        for at, task in work.items():
            pl.when(n == at)(task)
        return 0

    lax.fori_loop(0, ep + 4, step, 0)

    pair(mt, m_half, md_s, md_r, 0).wait_recv()
    whole = m_half[0] + mt[t]
    for k in range(1, ys):
        my_copy(k).wait_recv()
        whole = whole + m_in[k].astype(f32)
    mo_ref[...] = rms_scale(whole, ms_ref[...]).astype(bf16)
    pair(st, e_half, ed_s, ed_r, 0).wait_recv()
    whole = e_half[0] + st[t]
    for k in range(1, ys):
        ey_copy(k).wait_recv()
        whole = whole + e_in[k]
    total[...] = whole

    def arrive(i, _):
        b_copy(i).wait()
        return 0

    lax.fori_loop(1, ep, arrive, 0)
    flat = back[...].reshape(-1, dq)
    routed = None
    for k in range(top):
        term = weights[:, k : k + 1] * jnp.dot(picks[k], flat, preferred_element_type=f32)
        routed = term if routed is None else routed + term
    r_buf[...] = routed.reshape(tp, each, dq)
    for i in range(1, tp):
        r_copy(i).start()
    mine = pl.ds(pl.multiple_of(t * dq, dq), dq)
    total[:, mine] = total[:, mine] + r_buf[t]
    for i in range(1, tp):
        r_copy(i).wait()
        q = lax.rem(t + tp - i, tp)
        cols = pl.ds(pl.multiple_of(q * dq, dq), dq)
        total[:, cols] = total[:, cols] + r_in[q]
    eo_ref[...] = rms_scale(total[...], es_ref[...]).astype(bf16)

    def settle(i, _):
        for k in range(1, ys):
            y_copy(k, i).wait_send()
            hy_copy(k, i).wait_send()
        for k in range(ys):
            c_copy(k, i).wait_send()
            hc_copy(k, i).wait_send()

        @pl.when(i > 0)
        def _():
            z_copy(i).wait_send()

        return 0

    lax.fori_loop(0, ep, settle, 0)
    for k in range(ys):
        pair(mt, m_half, md_s, md_r, k).wait_send()
        pair(st, e_half, ed_s, ed_r, k).wait_send()
    for k in range(1, ys):
        my_copy(k).wait_send()
        ey_copy(k).wait_send()


def dma(*shape):
    return pltpu.SemaphoreType.DMA(shape)


def layer(ep, tp, small, large):
    outq, normed, _, _, ig = small[:5]
    picks = small[7]
    _, cap, dq = outq.shape
    rows, depth = normed.shape
    width = large[0].shape[1]
    hf, hs = large[3].shape[1], large[6].shape[1]
    each, ys, top = rows // tp, tp // 2, picks.shape[0]
    V = pltpu.VMEM
    return pl.pallas_call(
        functools.partial(layer_kernel, ep, tp, top),
        out_shape=[jax.ShapeDtypeStruct((each, depth), bf16)] * 2,
        in_specs=[pl.BlockSpec(memory_space=V)] * len(small)
        + [pl.BlockSpec(memory_space=pl.ANY)] * len(large),
        out_specs=[pl.BlockSpec(memory_space=V)] * 2,
        scratch_shapes=[
            V((depth, width), bf16),
            V((depth, hf), bf16),
            V((depth, hf), bf16),
            V((tp, hf, dq), bf16),
            V((hs, depth), bf16),
            V((tp, ep, cap, dq), bf16),
            V((tp, ep, cap, hf), bf16),
            V((ep, cap, dq), bf16),
            V((ep, cap, dq), bf16),
            V((tp, each, depth), f32),
            V((tp, each, depth), f32),
            V((ys, each, depth), f32),
            V((ys, each, depth), f32),
            V((ys, each, depth), bf16),
            V((ys, each, depth), bf16),
            V((ys, each, depth), f32),
            V((tp, each, dq), f32),
            V((tp, each, dq), f32),
            V((each, depth), f32),
            V((rows, width), f32),
            V((rows, width), f32),
            V((rows, width), f32),
            V((halo_rows + rows, width), f32),
            V((halo_rows, width), bf16),
            V((halo_rows, width), bf16),
            V((8, width), f32),
            V((ep, 8, width), f32),
            V((rows, width), bf16),
            dma(9 + tp), pltpu.SemaphoreType.DMA, pltpu.SemaphoreType.DMA, dma(ep), dma(ep),
            dma(ep), dma(ep),
            dma(ys, ep), dma(ys, ep),
            dma(ys, ep), dma(ys, ep),
            dma(ys, ep), dma(ys, ep),
            dma(ys, ep), dma(ys, ep),
            dma(tp), dma(tp),
            dma(ep), dma(ep),
            dma(ys), dma(ys), dma(ys), dma(ys),
            dma(ys), dma(ys), dma(ys), dma(ys),
            dma(tp), dma(tp),
        ],
        compiler_params=pltpu.CompilerParams(
            collective_id=0, has_side_effects=True, vmem_limit_bytes=67000000
        ),
        name="layer",
    )(*small, *large)


def body(
    mixer_rows, mixer_gain, gate_proj, input_proj, conv_taps, input_gates, decay_gates,
    decay_offset, out_proj, mixer_scale, expert_rows, expert_gain, route_ids, route_weights,
    expert_gate, expert_up, expert_down, shared_gate, shared_up, shared_down, expert_scale,
):
    ep, tp = lax.axis_size("ep"), lax.axis_size("tp")
    me, t = lax.axis_index("ep"), lax.axis_index("tp")
    tokens, width = expert_rows.shape
    top = route_ids.shape[1]
    cap = tokens * top * 3 // (2 * ep)
    dq = width // tp

    expert_normed = rms_scale(expert_rows, expert_gain).astype(bf16)
    offset_ids = lax.rem(route_ids + (ep - me), ep)
    indicator = jnp.sum(
        (offset_ids[:, :, None] == jnp.arange(ep, dtype=jnp.int32)).astype(f32), axis=1
    )
    below = (
        jnp.arange(tokens)[:, None] > jnp.arange(tokens)[None, :]
    ).astype(bf16)
    earlier = jnp.dot(below, indicator.astype(bf16), preferred_element_type=f32)
    chosen = (offset_ids[:, :, None] == jnp.arange(ep, dtype=jnp.int32)).astype(f32)
    position = jnp.sum(chosen * earlier[:, None, :], axis=2).astype(jnp.int32)
    slot_ids = offset_ids * cap + position
    slots = jnp.arange(ep * cap, dtype=jnp.int32)
    picks = [(slot_ids[:, k][:, None] == slots[None, :]).astype(bf16) for k in range(top)]
    placed = sum(picks[1:], picks[0])
    quarter = lax.dynamic_slice_in_dim(expert_normed, t * dq, dq, axis=1)
    outq = lax.dot_general(
        placed, quarter, (((0,), (0,)), ((), ())), preferred_element_type=f32
    ).astype(bf16).reshape(ep, cap, dq)
    normed = rms_scale(mixer_rows, mixer_gain).astype(bf16)
    soft = jax.nn.softplus(-decay_offset).reshape(1, -1)
    small = (
        outq, normed, expert_normed, conv_taps, input_gates, decay_gates, soft, jnp.stack(picks),
        route_weights, mixer_scale.reshape(1, -1), expert_scale.reshape(1, -1),
    )
    large = (
        input_proj, gate_proj, out_proj, expert_gate[0], expert_up[0], expert_down[0],
        shared_gate, shared_up, shared_down,
    )
    return tuple(layer(ep, tp, small, large))


def solution(mesh):
    placed = (
        P("ep", None),
        P(),
        P(None, "tp"),
        P(None, "tp"),
        P(None, "tp"),
        P("tp", None, None),
        P("tp", None, None),
        P("tp"),
        P("tp", None),
        P(),
        P("ep", None),
        P(),
        P("ep", None),
        P("ep", None),
        P("ep", None, "tp"),
        P("ep", None, "tp"),
        P("ep", "tp", None),
        P(None, "tp"),
        P(None, "tp"),
        P("tp", None),
        P(),
    )
    return jax.shard_map(
        body,
        mesh=mesh,
        in_specs=placed,
        out_specs=(P(("ep", "tp"), None), P(("ep", "tp"), None)),
        check_vma=False,
    )
```

```python
import functools

import jax
import jax.numpy as jnp
from jax import lax
from jax.experimental import pallas as pl
from jax.experimental.pallas import tpu as pltpu
from jax.sharding import PartitionSpec as P

eps = 1e-06
lru_power = 8.0
halo_rows = 16
MESH = pl.DeviceIdType.MESH
f32 = jnp.float32
bf16 = jnp.bfloat16


def rms_scale(values, scale):
    floats = values.astype(f32)
    return floats * lax.rsqrt(jnp.mean(floats * floats, axis=-1, keepdims=True) + eps) * scale


def remote(src, dst, send_sem, recv_sem, ep_at, tp_at):
    return pltpu.make_async_remote_copy(
        src_ref=src,
        dst_ref=dst,
        send_sem=send_sem,
        recv_sem=recv_sem,
        device_id=(ep_at, tp_at),
        device_id_type=MESH,
    )


def greet(peers):
    barrier = pltpu.get_barrier_semaphore()
    for ep_at, tp_at in peers:
        pl.semaphore_signal(barrier, inc=1, device_id=(ep_at, tp_at), device_id_type=MESH)
    pl.semaphore_wait(barrier, len(peers))


def expm1_neg(y):
    series = y * (1 + y / 2 * (1 + y / 3 * (1 + y / 4 * (1 + y / 5 * (1 + y / 6 * (1 + y / 7))))))
    return jnp.where(y > -0.35, series, jnp.exp(y) - 1.0)


def layer_kernel(
    ep, tp, top,
    slots, slots_t, taps_ref, ig_ref, dg_ref, soft_ref, weights, mg_ref, xg_ref, ms_ref, es_ref,
    rows_hbm, tokens_hbm, ip_hbm, gp_hbm, op_hbm, eg_hbm, eu_hbm, ed, sg_hbm, su_hbm, sd_hbm,
    mo_ref, eo_ref,
    outq, normed, en, e_out, r_out, r_near,
    w1, eg, eu, wd, sd, recv, hid, ret, back, mt, st, m_half, e_half, m_out, m_in, e_in,
    r_buf, r_in, total, gate, a_buf, b_buf, ext, tail, halo, ends, got, gated,
    load_sem, halo_send, halo_recv, end_send, end_recv,
    z_s, z_r, y_s, y_r, c_s, c_r, hy_s, hy_r, hc_s, hc_r, w_s, w_r, b_s, b_r,
    md_s, md_r, ed_s, ed_r, my_s, my_r, ey_s, ey_r, r_s, r_r,
):
    me, t = lax.axis_index("ep"), lax.axis_index("tp")
    ys = tp // 2
    y, c = t // 2, lax.rem(t, 2)
    mate = y * 2 + 1 - c
    dq = outq.shape[2]
    rows, width = ext.shape[0] - halo_rows, ext.shape[1]
    each = rows // tp
    blocks, bw = ig_ref.shape[0], ig_ref.shape[1]
    sh_width = sd.shape[0]

    def at_y(k):
        return lax.rem(y + k, ys)

    def up(k):
        return at_y(k) * 2 + c

    def down_of(k, core):
        return lax.rem(y + ys - k, ys) * 2 + core

    greet(
        [(lax.rem(me + i, ep), t) for i in range(1, ep)]
        + [(me, lax.rem(t + i, tp)) for i in range(1, tp)]
    )

    def z_copy(i):
        return remote(
            outq.at[i], recv.at[t, i], z_s.at[i], z_r.at[i], lax.rem(me + i, ep), t
        )

    def y_copy(k, i):
        return remote(recv.at[t, i], recv.at[t, i], y_s.at[k, i], y_r.at[k, i], me, up(k))

    def c_copy(k, i):
        q = down_of(k, c)
        return remote(recv.at[q, i], recv.at[q, i], c_s.at[k, i], c_r.at[k, i], me, mate)

    def hy_copy(k, i):
        return remote(hid.at[t, i], hid.at[t, i], hy_s.at[k, i], hy_r.at[k, i], me, up(k))

    def hc_copy(k, i):
        q = down_of(k, c)
        return remote(hid.at[q, i], hid.at[q, i], hc_s.at[k, i], hc_r.at[k, i], me, mate)

    def w_copy(i):
        q = lax.rem(t + i, tp)
        return remote(
            ed.at[:, pl.ds(pl.multiple_of(q * dq, dq), dq)], wd.at[t],
            w_s.at[i], w_r.at[i], me, q,
        )

    def b_copy(i):
        return remote(
            ret.at[i], back.at[i], b_s.at[i], b_r.at[i], lax.rem(me + ep - i, ep), t
        )

    def halo_copy():
        return remote(tail, halo, halo_send, halo_recv, lax.rem(me + 1, ep), t)

    def end_copy(i):
        return remote(ends, got.at[i], end_send.at[i], end_recv.at[i], lax.rem(me + i, ep), t)

    def pair(ref, half, s, r, k):
        return remote(ref.at[at_y(k) * 2 + 1 - c], half.at[k], s.at[k], r.at[k], me, mate)

    def my_copy(k):
        return remote(m_out.at[k], m_in.at[k], my_s.at[k], my_r.at[k], me, up(k))

    def ey_copy(k):
        return remote(e_out.at[k], e_in.at[k], ey_s.at[k], ey_r.at[k], me, up(k))

    def r_copy(k, core):
        j, q = 2 * k + core, at_y(k) * 2 + lax.rem(c + core, 2)
        if k == 0:
            return remote(r_buf.at[q], r_near, r_s.at[j], r_r.at[j], me, q)
        return remote(r_out.at[q], r_in.at[t], r_s.at[j], r_r.at[j], me, q)

    def load(src, dst, at):
        return pltpu.make_async_copy(src, dst, load_sem.at[at])

    for i in range(1, tp):
        w_copy(i).start()
    tokens_load, rows_load = load(tokens_hbm, en, 0), load(rows_hbm, normed, 9 + tp)
    tokens_load.start()
    rows_load.start()
    ip_load = load(ip_hbm, w1, 1)
    ip_load.start()
    eg_load, eu_load = load(eg_hbm, eg, 2), load(eu_hbm, eu, 3)
    eg_load.start()
    eu_load.start()
    wd_load = load(ed.at[:, pl.ds(pl.multiple_of(t * dq, dq), dq)], wd.at[t], 4)
    wd_load.start()
    sd_load = load(sd_hbm, sd, 5)
    sd_load.start()

    def normalize(ref, gain):
        def some(r, _):
            at = pl.ds(pl.multiple_of(r * 32, 32), 32)
            ref[at, :] = rms_scale(ref[at, :], gain[...]).astype(bf16)
            return 0

        lax.fori_loop(0, rows // 32, some, 0)

    tokens_load.wait()
    normalize(en, xg_ref)
    cap = outq.shape[1]
    mine = pl.ds(pl.multiple_of(t * dq, dq), dq)

    def place(i):
        spot = lax.broadcasted_iota(jnp.int32, (cap, rows), 0) + i * cap
        hot = slots_t[0:1, :] == spot
        for k in range(1, top):
            hot = hot | (slots_t[k : k + 1, :] == spot)
        return hot.astype(f32).astype(bf16)

    def dispatch(i, _):
        outq[i] = jnp.dot(place(i), en[:, mine], preferred_element_type=f32).astype(bf16)
        z_copy(i).start()
        return 0

    lax.fori_loop(1, ep, dispatch, 0)
    local = place(0)
    for q in range(tp):
        recv[q, 0] = jnp.dot(
            local, en[:, pl.ds(q * dq, dq)], preferred_element_type=f32
        ).astype(bf16)
    rows_load.wait()
    normalize(normed, mg_ref)
    sg_load = load(sg_hbm, w1.at[:, pl.ds(0, sh_width)], 6)
    su_load = load(su_hbm, w1.at[:, pl.ds(sh_width, sh_width)], 7)
    gp_load = load(gp_hbm, w1, 8)
    op_loads = [
        load(op_hbm.at[:, pl.ds(q * dq, dq)], w1.at[pl.ds(q * width, width), :], 9 + q)
        for q in range(tp)
    ]

    def project():
        ip_load.wait()

        def columns(j, _):
            cols = pl.ds(pl.multiple_of(j * bw, bw), bw)
            piece = jnp.dot(normed[...], w1[:, cols], preferred_element_type=f32).astype(bf16)
            ext[pl.ds(halo_rows, rows), cols] = piece.astype(f32)
            tail[:, cols] = piece[rows - halo_rows :]
            return 0

        lax.fori_loop(0, width // bw, columns, 0)
        halo_copy().start()
        sg_load.start()
        su_load.start()

    def shared():
        sg_load.wait()
        su_load.wait()
        g = jnp.dot(en[...], w1[:, pl.ds(0, sh_width)], preferred_element_type=f32)
        u = jnp.dot(en[...], w1[:, pl.ds(sh_width, sh_width)], preferred_element_type=f32)
        hidden = (jax.nn.silu(g) * u).astype(bf16)
        gp_load.start()
        sd_load.wait()
        for q in range(tp):
            cols = pl.ds(q * dq, dq)
            piece = jnp.dot(hidden, sd[:, cols], preferred_element_type=f32)
            st[:, :, cols] = piece.reshape(tp, each, dq)
        for k in range(ys):
            pair(st, e_half, ed_s, ed_r, k).start()

    def gate_step():
        gp_load.wait()

        def columns(j, _):
            cols = pl.ds(pl.multiple_of(j * bw, bw), bw)
            piece = jnp.dot(normed[...], w1[:, cols], preferred_element_type=f32)
            gate[:, cols] = jax.nn.gelu(piece)
            return 0

        lax.fori_loop(0, width // bw, columns, 0)
        for one in op_loads:
            one.start()

    def convolve():
        halo_copy().wait()
        ext[pl.ds(0, halo_rows), :] = jnp.where(me == 0, 0.0, halo[...].astype(f32))
        taps = taps_ref.shape[0]
        base = halo_rows - (taps - 1)
        first = (lax.broadcasted_iota(jnp.int32, (rows, bw), 0) == 0) & (me == 0)
        for b in range(blocks):
            cols = pl.ds(b * bw, bw)
            acc = taps_ref[0:1, cols] * ext[pl.ds(base, rows), cols]
            for k in range(1, taps):
                acc = acc + taps_ref[k : k + 1, cols] * ext[pl.ds(base + k, rows), cols]
            conv = acc.astype(bf16)
            ig = jax.nn.sigmoid(jnp.dot(conv, ig_ref[b], preferred_element_type=f32))
            dg = jax.nn.sigmoid(jnp.dot(conv, dg_ref[b], preferred_element_type=f32))
            ld = -lru_power * dg * soft_ref[0:1, cols]
            scale = jnp.where(first, 1.0, jnp.sqrt(-expm1_neg(2.0 * ld)))
            a_buf[:, cols] = jnp.exp(ld)
            b_buf[:, cols] = scale * ig * conv.astype(f32)

    def scan():
        row = lax.broadcasted_iota(jnp.int32, (8, width), 0)

        def block(r, carry):
            pc, sc = carry
            at = pl.ds(pl.multiple_of(r * 8, 8), 8)
            a, b = a_buf[at, :], b_buf[at, :]
            for sh in (1, 2, 4):
                keep = row >= sh
                b = jnp.where(keep, b + a * pltpu.roll(b, sh, 0), b)
                a = jnp.where(keep, a * pltpu.roll(a, sh, 0), a)
            b = b + a * sc
            a = a * pc
            a_buf[at, :] = a
            b_buf[at, :] = b
            return a[7:8, :], b[7:8, :]

        pl_last, s_last = lax.fori_loop(
            0, rows // 8, block, (jnp.ones((1, width), f32), jnp.zeros((1, width), f32))
        )
        ends[...] = jnp.where(row == 0, pl_last, s_last)
        for i in range(1, ep):
            end_copy(i).start()

    def carry_in():
        for i in range(1, ep):
            end_copy(i).wait()
        carry = jnp.zeros((1, width), f32)
        for i in range(ep - 1, 0, -1):
            carry = jnp.where(me >= i, got[i, 0:1, :] * carry + got[i, 1:2, :], carry)

        def finish(r, _):
            at = pl.ds(pl.multiple_of(r * 16, 16), 16)
            gated[at, :] = (gate[at, :] * (b_buf[at, :] + a_buf[at, :] * carry)).astype(bf16)
            return 0

        lax.fori_loop(0, rows // 16, finish, 0)

    def project_out():
        for one in op_loads:
            one.wait()
        for q in range(tp):
            piece = jnp.dot(
                gated[...], w1[pl.ds(q * width, width), :], preferred_element_type=f32
            )
            mt[:, :, pl.ds(q * dq, dq)] = piece.reshape(tp, each, dq)
        for k in range(ys):
            pair(mt, m_half, md_s, md_r, k).start()

    def shared_half():
        for k in range(1, ys):
            pair(st, e_half, ed_s, ed_r, k).wait_recv()
            e_out[k] = (e_half[k] + st[up(k)]).astype(bf16)
            ey_copy(k).start()

    def mixer_half():
        for k in range(1, ys):
            pair(mt, m_half, md_s, md_r, k).wait_recv()
            m_out[k] = (m_half[k] + mt[up(k)]).astype(bf16)
            my_copy(k).start()

    work = {
        0: project, 1: shared, 2: gate_step, 3: convolve, 4: scan, 5: carry_in, 6: project_out,
        ep - 1: shared_half, ep + 2: mixer_half,
    }

    def step(n, _):
        @pl.when((n > 0) & (n < ep))
        def _():
            i = n
            z_copy(i).wait_recv()
            for k in range(1, ys):
                y_copy(k, i).start()
            c_copy(0, i).start()

        @pl.when((n >= 2) & (n < ep + 1))
        def _():
            i = n - 1
            for k in range(1, ys):
                y_copy(k, i).wait_recv()
                c_copy(k, i).start()

        @pl.when(n == 2)
        def _():
            eg_load.wait()
            eu_load.wait()

        @pl.when((n >= 2) & (n < ep + 2))
        def _():
            i = n - 2

            @pl.when(i > 0)
            def _():
                for k in range(ys):
                    c_copy(k, i).wait_recv()

            gate_sum = up_sum = None
            for q in range(tp):
                x = recv[q, i]
                span = pl.ds(q * dq, dq)
                g = jnp.dot(x, eg[span, :], preferred_element_type=f32)
                u = jnp.dot(x, eu[span, :], preferred_element_type=f32)
                gate_sum = g if gate_sum is None else gate_sum + g
                up_sum = u if up_sum is None else up_sum + u
            hid[t, i] = (jax.nn.silu(gate_sum) * up_sum).astype(bf16)
            for k in range(1, ys):
                hy_copy(k, i).start()
            hc_copy(0, i).start()

        @pl.when((n >= 3) & (n < ep + 3))
        def _():
            i = n - 3
            for k in range(1, ys):
                hy_copy(k, i).wait_recv()
                hc_copy(k, i).start()

        @pl.when(n == 4)
        def _():
            wd_load.wait()
            for i in range(1, tp):
                w_copy(i).wait()

        @pl.when(n >= 4)
        def _():
            i = n - 4
            for k in range(ys):
                hc_copy(k, i).wait_recv()
            out = jnp.dot(hid[0, i], wd[0], preferred_element_type=f32)
            for q in range(1, tp):
                out = out + jnp.dot(hid[q, i], wd[q], preferred_element_type=f32)

            @pl.when(i == 0)
            def _():
                back[0] = out.astype(bf16)

            @pl.when(i > 0)
            def _():
                ret[i] = out.astype(bf16)
                b_copy(i).start()

        for at, task in work.items():
            pl.when(n == at)(task)
        return 0

    lax.fori_loop(0, ep + 4, step, 0)

    pair(mt, m_half, md_s, md_r, 0).wait_recv()
    whole = m_half[0] + mt[t]
    for k in range(1, ys):
        my_copy(k).wait_recv()
        whole = whole + m_in[k].astype(f32)
    mo_ref[...] = rms_scale(whole, ms_ref[...]).astype(bf16)
    pair(st, e_half, ed_s, ed_r, 0).wait_recv()
    whole = e_half[0] + st[t]
    for k in range(1, ys):
        ey_copy(k).wait_recv()
        whole = whole + e_in[k].astype(f32)
    total[...] = whole

    def arrive(i, _):
        b_copy(i).wait()
        return 0

    lax.fori_loop(1, ep, arrive, 0)
    flat = back[...].reshape(-1, dq)
    spot = lax.broadcasted_iota(jnp.int32, (rows, ep * cap), 1)
    routed = None
    for k in range(top):
        pick = (slots[:, k : k + 1] == spot).astype(f32).astype(bf16)
        term = weights[:, k : k + 1] * jnp.dot(pick, flat, preferred_element_type=f32)
        routed = term if routed is None else routed + term
    routed = routed.reshape(tp, each, dq)
    r_out[...] = routed.astype(bf16)
    for k in range(1, ys):
        for core in range(2):
            r_copy(k, core).start()
    r_buf[...] = routed
    r_copy(0, 1).start()
    total[:, mine] = total[:, mine] + r_buf[t]
    r_copy(0, 1).wait()
    near = pl.ds(pl.multiple_of(mate * dq, dq), dq)
    total[:, near] = total[:, near] + r_near[...]
    for k in range(1, ys):
        for core in range(2):
            r_copy(k, core).wait()
            q = down_of(k, lax.rem(c + core, 2))
            cols = pl.ds(pl.multiple_of(q * dq, dq), dq)
            total[:, cols] = total[:, cols] + r_in[q].astype(f32)
    eo_ref[...] = rms_scale(total[...], es_ref[...]).astype(bf16)

    def settle(i, _):
        for k in range(1, ys):
            hy_copy(k, i).wait_send()
        for k in range(ys):
            hc_copy(k, i).wait_send()

        @pl.when(i > 0)
        def _():
            for k in range(1, ys):
                y_copy(k, i).wait_send()
            for k in range(ys):
                c_copy(k, i).wait_send()
            z_copy(i).wait_send()

        return 0

    lax.fori_loop(0, ep, settle, 0)
    for k in range(ys):
        pair(mt, m_half, md_s, md_r, k).wait_send()
        pair(st, e_half, ed_s, ed_r, k).wait_send()
    for k in range(1, ys):
        my_copy(k).wait_send()
        ey_copy(k).wait_send()


def dma(*shape):
    return pltpu.SemaphoreType.DMA(shape)


def layer(ep, tp, small, large):
    rows, depth = large[0].shape
    width = large[2].shape[1]
    hf, hs = large[5].shape[1], large[8].shape[1]
    top = small[0].shape[1]
    each, ys, dq = rows // tp, tp // 2, depth // tp
    cap = rows * top * 3 // (2 * ep)
    V = pltpu.VMEM
    return pl.pallas_call(
        functools.partial(layer_kernel, ep, tp, top),
        out_shape=[jax.ShapeDtypeStruct((each, depth), bf16)] * 2,
        in_specs=[pl.BlockSpec(memory_space=V)] * len(small)
        + [pl.BlockSpec(memory_space=pl.ANY)] * len(large),
        out_specs=[pl.BlockSpec(memory_space=V)] * 2,
        scratch_shapes=[
            V((ep, cap, dq), bf16),
            V((rows, depth), bf16),
            V((rows, depth), bf16),
            V((ys, each, depth), bf16),
            V((tp, each, dq), bf16),
            V((each, dq), f32),
            V((depth, width), bf16),
            V((depth, hf), bf16),
            V((depth, hf), bf16),
            V((tp, hf, dq), bf16),
            V((hs, depth), bf16),
            V((tp, ep, cap, dq), bf16),
            V((tp, ep, cap, hf), bf16),
            V((ep, cap, dq), bf16),
            V((ep, cap, dq), bf16),
            V((tp, each, depth), f32),
            V((tp, each, depth), f32),
            V((ys, each, depth), f32),
            V((ys, each, depth), f32),
            V((ys, each, depth), bf16),
            V((ys, each, depth), bf16),
            V((ys, each, depth), bf16),
            V((tp, each, dq), f32),
            V((tp, each, dq), bf16),
            V((each, depth), f32),
            V((rows, width), f32),
            V((rows, width), f32),
            V((rows, width), f32),
            V((halo_rows + rows, width), f32),
            V((halo_rows, width), bf16),
            V((halo_rows, width), bf16),
            V((8, width), f32),
            V((ep, 8, width), f32),
            V((rows, width), bf16),
            dma(10 + tp), pltpu.SemaphoreType.DMA, pltpu.SemaphoreType.DMA, dma(ep), dma(ep),
            dma(ep), dma(ep),
            dma(ys, ep), dma(ys, ep),
            dma(ys, ep), dma(ys, ep),
            dma(ys, ep), dma(ys, ep),
            dma(ys, ep), dma(ys, ep),
            dma(tp), dma(tp),
            dma(ep), dma(ep),
            dma(ys), dma(ys), dma(ys), dma(ys),
            dma(ys), dma(ys), dma(ys), dma(ys),
            dma(tp), dma(tp),
        ],
        compiler_params=pltpu.CompilerParams(
            collective_id=0, has_side_effects=True, vmem_limit_bytes=67000000
        ),
        name="layer",
    )(*small, *large)


def body(
    mixer_rows, mixer_gain, gate_proj, input_proj, conv_taps, input_gates, decay_gates,
    decay_offset, out_proj, mixer_scale, expert_rows, expert_gain, route_ids, route_weights,
    expert_gate, expert_up, expert_down, shared_gate, shared_up, shared_down, expert_scale,
):
    ep, tp = lax.axis_size("ep"), lax.axis_size("tp")
    me = lax.axis_index("ep")
    tokens = expert_rows.shape[0]
    top = route_ids.shape[1]
    cap = tokens * top * 3 // (2 * ep)
    offset_ids = lax.rem(route_ids + (ep - me), ep)
    indicator = jnp.sum(
        (offset_ids[:, :, None] == jnp.arange(ep, dtype=jnp.int32)).astype(f32), axis=1
    )
    below = (
        jnp.arange(tokens)[:, None] > jnp.arange(tokens)[None, :]
    ).astype(bf16)
    earlier = jnp.dot(below, indicator.astype(bf16), preferred_element_type=f32)
    chosen = (offset_ids[:, :, None] == jnp.arange(ep, dtype=jnp.int32)).astype(f32)
    position = jnp.sum(chosen * earlier[:, None, :], axis=2).astype(jnp.int32)
    slot_ids = offset_ids * cap + position
    soft = jax.nn.softplus(-decay_offset).reshape(1, -1)
    gains = [x.reshape(1, -1) for x in (mixer_gain, expert_gain, mixer_scale, expert_scale)]
    small = (
        slot_ids, slot_ids.T, conv_taps, input_gates, decay_gates, soft, route_weights, *gains,
    )
    large = (
        mixer_rows, expert_rows, input_proj, gate_proj, out_proj, expert_gate[0], expert_up[0], expert_down[0],
        shared_gate, shared_up, shared_down,
    )
    return tuple(layer(ep, tp, small, large))


def solution(mesh):
    placed = (
        P("ep", None),
        P(),
        P(None, "tp"),
        P(None, "tp"),
        P(None, "tp"),
        P("tp", None, None),
        P("tp", None, None),
        P("tp"),
        P("tp", None),
        P(),
        P("ep", None),
        P(),
        P("ep", None),
        P("ep", None),
        P("ep", None, "tp"),
        P("ep", None, "tp"),
        P("ep", "tp", None),
        P(None, "tp"),
        P(None, "tp"),
        P("tp", None),
        P(),
    )
    return jax.shard_map(
        body,
        mesh=mesh,
        in_specs=placed,
        out_specs=(P(("ep", "tp"), None), P(("ep", "tp"), None)),
        check_vma=False,
    )
```
